512 devices in a mesh: sp: 32 (over z, core), tp: 16 (over y, x).
Axes of the slice: x: 4, y: 4, z: 16, core: 2. Of those that a mesh axis runs over, the one named last changes fastest.
Arguments:
- mix_values: bfloat16 [4096, 4096], P('sp', 'tp'), may hold values from -6 to 6
- mix_gate: bfloat16 [4096, 4096], P('sp', 'tp'), may hold values from -6 to 6
- input_keys: bfloat16 [4096, 2048], P('sp', 'tp'), may hold values from -0.22460938 to 0.22460938
- output_keys: bfloat16 [4096, 2048], P('sp', 'tp'), may hold values from -0.22460938 to 0.22460938
- step_sizes: float32 [4096, 64], P('sp', 'tp'), may hold values from 0.1 to 8
- decay_rates: float32 [64], P('tp'), may hold values from 1.2207031e-05 to 0.03
- out_proj: bfloat16 [2048, 4096], P('sp', 'tp'), may hold values from -0.09375 to 0.09375
- expert_inputs: bfloat16 [4096, 2048], P('sp'), may hold values from -20 to 20
- stream_grad: bfloat16 [4096, 2048], P('sp'), may hold values from -6 to 6
- routes: int32 [4096, 2], P('sp'), may hold values from 0 to 31, all different within a row; in each aligned block of 128 rows (0 to 127, 128 to 255, ...) at most 12 rows name the same one
- route_weights: float32 [4096, 2], P('sp'), may hold values from 0.1 to 0.9
- gate_proj: bfloat16 [32, 2048, 2048], P('sp', 'tp'), may hold values from -0.125 to 0.125
- up_proj: bfloat16 [32, 2048, 2048], P('sp', 'tp'), may hold values from -0.125 to 0.125
- down_proj: bfloat16 [32, 2048, 2048], P('sp', 'tp'), may hold values from -0.125 to 0.125
Outputs:
- grad_gate_proj: bfloat16 [32, 2048, 2048], P('sp', 'tp')
- grad_up_proj: bfloat16 [32, 2048, 2048], P('sp', 'tp')
- grad_down_proj: bfloat16 [32, 2048, 2048], P('sp', 'tp')
- grad_out_proj: float32 [2048, 4096], P('sp', 'tp')
- grad_values: bfloat16 [4096, 4096], P('sp', 'tp')
- grad_gate: bfloat16 [4096, 4096], P('sp', 'tp')
- grad_input_keys: bfloat16 [4096, 2048], P('sp', 'tp')
- grad_output_keys: bfloat16 [4096, 2048], P('sp', 'tp')
- grad_steps: float32 [4096, 64], P('sp', 'tp')
The draws below stay inside these ranges and needn't reach their ends.
Inputs may be any that keep to these rules, and one draw needn't show every extreme that they name: In the rows of one device no expert is named by more than 12 routes, and on some devices one expert is named by exactly 12; the 2 routes of a token name different experts.
All inputs are finite; a program needn't handle non-finite values.
Results may differ from the reference program's by a relative error of at most 0.025.
Values may be sent and summed in bfloat16 or wider, within the bound.
A program may use at most 64 MiB of HBM per device.

```python
import math
import jax
import jax.numpy as jnp
import numpy as np
from jax import lax

D = 2048
HEAD_DIM = 64
HEADS = 64
GROUPS = 16
NSTATE = 128
BLOCK = 128
F = 2048
TOPK = 2
TOK_DEV = 128
DI = 4096
EXPERTS = 32
TOKENS = 4096
CAP = 12
N_SP = 32


def draw_decay_rates(key, part):
    choose_key, fast_key, slow_key = jax.random.split(jax.random.fold_in(key, 11), 3)
    share = 0.5
    fast_heads = jax.random.uniform(choose_key, (HEADS,), jnp.float32) < share
    fast_rate = jnp.exp(jax.random.uniform(fast_key, (HEADS,), jnp.float32, jnp.log(0.01), jnp.log(0.03)))
    slow_rate = jnp.exp(jax.random.uniform(slow_key, (HEADS,), jnp.float32, jnp.log(0.05), jnp.log(0.5))) / TOKENS
    return jnp.where(fast_heads, fast_rate, slow_rate).astype(jnp.float32)


def draw_step_sizes(key, part):
    base_key, block_key = jax.random.split(jax.random.fold_in(key, 23), 2)
    base = jnp.exp(jax.random.uniform(base_key, (TOKENS, HEADS), jnp.float32, -0.7, 0.7))
    factor = jnp.exp(jax.random.uniform(block_key, (TOKENS // BLOCK, 1), jnp.float32, jnp.log(0.4), jnp.log(2.5)))
    return (base * jnp.repeat(factor, BLOCK, axis=0)).astype(jnp.float32)


def draw_expert_inputs(key, part):
    base_key, pick_key, scale_key = jax.random.split(jax.random.fold_in(key, 37), 3)
    base = jnp.clip(jax.random.normal(base_key, (TOKENS, D), jnp.float32), -2.5, 2.5)
    picked = jax.random.uniform(pick_key, (TOKENS, 1), jnp.float32) < 0.0625
    row_scale = jax.random.uniform(scale_key, (TOKENS, 1), jnp.float32, 5.0, 8.0)
    return (base * jnp.where(picked, row_scale, 1.0)).astype(jnp.bfloat16)


def with_spikes(array, key, source, target, parts, factor):
    owner, partner = [(jnp.arange(array.shape[axis_at]) // (array.shape[axis_at] // parts)).reshape([-1 if axis == axis_at else 1 for axis in range(array.ndim)]) for axis_at in (source, target)]
    chosen = jax.random.permutation(key, parts)[partner]
    strong = (owner == chosen) | (owner == (partner + parts // 2) % parts)
    return jnp.where(strong, factor * array, array)


def levels(stream_key, dims, cuts, low, top_value):
    def one(position, parts):
        heights = jax.random.uniform(jax.random.fold_in(jax.random.fold_in(stream_key, 6), position), (parts,), jnp.float32, low / len(cuts), top_value / len(cuts))
        return jnp.repeat(jnp.exp(heights), dims[position] // parts).reshape((-1,) + (1,) * (len(dims) - position - 1))

    loudness = one(*cuts[0])
    for cut in cuts[1:]:
        loudness = loudness * one(*cut)
    return loudness


def assign_block(rng, own, number, rows, number_of, top, bound, skew):
    sequence = jax.random.permutation(rng, number_of)
    crowded, usual = shares(number_of, rows * top, bound, skew, True), shares(number_of, rows * top, bound, skew, False)
    places = jnp.arange(number_of)

    def named(lengths, turn):
        used = int((lengths > 0).sum())
        fixed = max(1, used // 4)
        moved = fixed + (places - fixed + turn * (used - fixed)) % max(1, number_of - fixed)
        return jnp.zeros((number_of,), jnp.int32).at[sequence[jnp.where(places < fixed, places, moved)]].set(jnp.asarray(lengths, jnp.int32))

    lengths = jnp.where(number % 4 == 0, named(crowded, number // 4), named(usual, number - number // 4 - 1))
    mixed = jax.random.permutation(jax.random.fold_in(own, 3), number_of)
    donor, receiver = mixed[0:number_of // 2 * 2:2], mixed[1:number_of // 2 * 2:2]
    room = jnp.minimum(lengths[donor] - 1, bound - lengths[receiver]) // 2
    room = jnp.where((donor == sequence[0]) | (receiver == sequence[0]) | (lengths[receiver] == 0), 0, jnp.maximum(room, 0))
    moved = jax.random.randint(jax.random.fold_in(own, 4), (number_of // 2,), 0, 1 << 20) % (room + 1)
    lengths = lengths.at[donor].add(-moved).at[receiver].add(moved)
    members = jnp.searchsorted(jnp.cumsum(lengths), jnp.arange(rows * top), side="right").astype(jnp.int32)
    table = members.reshape(top, rows).T
    table = table[jax.random.permutation(jax.random.fold_in(own, 1), rows)]
    turn = jax.random.randint(jax.random.fold_in(own, 2), (rows, 1), 0, top)
    return jnp.take_along_axis(table, (jnp.arange(top)[None, :] + turn) % top, axis=1)


def shares(count, total, most, lean, full):
    weights = [(1 << 20) // math.isqrt(standing ** lean) + 1 for standing in range(1, count + 1)]
    largest = most if full else min(most, max(-(-total // count), total * weights[0] // sum(weights)))
    least = 1 if total - largest >= count - 1 else 0
    given, spare = [largest] + [least] * (count - 1), total - largest - least * (count - 1)
    while spare > 0:
        free = [i for i in range(1, count) if given[i] < largest] or [i for i in range(1, count) if given[i] < most]
        pool, budget = sum([weights[i] for i in free]), spare
        for i in free:
            addition = min(most - given[i], max(1, budget * weights[i] // pool), spare)
            given[i] = given[i] + addition
            spare = spare - addition
    return np.array(given)


def gaussian(stream_key, dims, width, limit, shards=(), held_as=jnp.bfloat16):
    factor_of = levels(stream_key, dims, shards, -0.22, 0.18) if shards else 1.0
    result = jax.random.normal(stream_key, dims, jnp.float32) * width * factor_of
    return jnp.minimum(jnp.maximum(result, -limit), limit).astype(held_as)


def heavy_noise(own_key, shape, width, most, cuts, heavy, kind=jnp.bfloat16):
    array = width * jax.random.normal(own_key, shape, jnp.float32)
    if cuts:
        array = array * levels(own_key, shape, cuts, -0.22, 0.18)
    return jnp.clip(with_spikes(array, jax.random.fold_in(own_key, 3), *heavy), -most, most).astype(kind)


def setup_inputs(seed: int = 0) -> dict:
    key_of = jax.random.split(jax.random.key(seed), 15)
    mix_values = gaussian(key_of[0], (TOKENS, DI), 1.0, 6.0, ((0, 32), (1, 16)))
    mix_gate = gaussian(key_of[1], (TOKENS, DI), 1.0, 6.0, ((0, 32), (1, 16)))
    input_keys = gaussian(key_of[2], (TOKENS, GROUPS * NSTATE), (0.3 * TOKENS ** -0.25), 0.22460938, ((0, 32), (1, 16)))
    output_keys = gaussian(key_of[3], (TOKENS, GROUPS * NSTATE), (0.3 * TOKENS ** -0.25), 0.22460938, ((0, 32), (1, 16)))
    step_sizes = draw_step_sizes(jax.random.fold_in(key_of[14], 71), 0)
    decay_rates = draw_decay_rates(jax.random.fold_in(key_of[14], 71), 0)
    out_proj = gaussian(key_of[6], (D, DI), DI ** -0.5, 0.09375, ((0, 32), (1, 16)))
    expert_inputs = draw_expert_inputs(jax.random.fold_in(key_of[14], 71), 0)
    stream_grad = heavy_noise(key_of[8], (TOKENS, D), 1.0, 6.0, ((0, 32),), (0, 1, 32, 2.75))
    routes_keys = jax.random.split(jax.random.fold_in(key_of[9], 1), TOKENS // TOK_DEV)
    routes_turns = jax.random.permutation(jax.random.fold_in(key_of[9], 3), TOKENS // TOK_DEV)
    routes = jax.vmap(lambda own, number: assign_block(jax.random.fold_in(key_of[9], 2), own, number, TOK_DEV, EXPERTS, TOPK, CAP, 1))(routes_keys, routes_turns).reshape((TOKENS, TOPK))
    route_weights = jnp.clip(0.1 + 0.79999997 * jax.random.uniform(key_of[10], (TOKENS, TOPK), jnp.float32) ** levels(key_of[10], (TOKENS, TOPK), ((0, 32),), -0.2, 0.2), 0.1, 0.9)
    gate_proj = gaussian(key_of[11], (EXPERTS, F, D), D ** -0.5, 0.125, ((0, 32), (1, 16)))
    up_proj = gaussian(key_of[12], (EXPERTS, F, D), D ** -0.5, 0.125, ((0, 32), (1, 16)))
    down_proj = gaussian(key_of[13], (EXPERTS, F, D), F ** -0.5, 0.125, ((0, 32), (1, 16)))
    return dict(mix_values=mix_values, mix_gate=mix_gate, input_keys=input_keys, output_keys=output_keys, step_sizes=step_sizes, decay_rates=decay_rates, out_proj=out_proj, expert_inputs=expert_inputs, stream_grad=stream_grad, routes=routes, route_weights=route_weights, gate_proj=gate_proj, up_proj=up_proj, down_proj=down_proj)


CLAMP_LIMIT = 7.0
SIGMOID_SCALE = 1.702
HIGHEST = lax.Precision.HIGHEST

def decay_span(head_values, in_keys, out_keys, head_steps, head_rates, start_state):
    length = head_values.shape[0]
    num_blocks = length // BLOCK
    causal_mask = jnp.tril(jnp.ones((BLOCK, BLOCK), dtype=bool))

    def advance(carry_state, block_data):
        block_values, block_in, block_out, block_steps = block_data
        log_decay = jnp.cumsum(-block_steps * head_rates, axis=0)
        weighted = block_values * block_steps[..., None]
        ordered = jnp.transpose(log_decay, (1, 2, 0))
        log_gaps = ordered[..., :, None] - ordered[..., None, :]
        mixing = jnp.where(causal_mask, jnp.exp(jnp.where(causal_mask, log_gaps, 0.0)), 0.0)
        scores = jnp.einsum('lgn,sgn->gls', block_out, block_in, precision=HIGHEST)
        within = jnp.einsum('grls,sgrp->lgrp', scores[:, None] * mixing, weighted, precision=HIGHEST)
        carried = jnp.einsum('lgn,grpn->lgrp', block_out, carry_state, precision=HIGHEST) * jnp.exp(log_decay)[..., None]
        to_end = jnp.exp(log_decay[-1] - log_decay)
        new_state = carry_state * jnp.exp(log_decay[-1])[..., None, None] + jnp.einsum('lgn,lgrp->grpn', block_in, weighted * to_end[..., None], precision=HIGHEST)
        return (new_state, within + carried)
    blocks = tuple((whole_array.reshape((num_blocks, BLOCK) + whole_array.shape[1:]) for whole_array in (head_values, in_keys, out_keys, head_steps)))
    last_state, block_outputs = lax.scan(advance, start_state, blocks)
    return (block_outputs.reshape(head_values.shape), last_state)

def expert_backward(in_rows, grad_rows, gate_weight, up_weight, down_weight):
    contract = (((1,), (1,)), ((), ()))
    across = (((0,), (0,)), ((), ()))
    gate_pre = lax.dot_general(in_rows, gate_weight, contract, preferred_element_type=jnp.float32)
    up_pre = lax.dot_general(in_rows, up_weight, contract, preferred_element_type=jnp.float32)
    gate_clamped = jnp.minimum(gate_pre, CLAMP_LIMIT)
    up_clamped = jnp.clip(up_pre, -CLAMP_LIMIT, CLAMP_LIMIT)
    gate_sigmoid = jax.nn.sigmoid(SIGMOID_SCALE * gate_clamped)
    activation = ((up_clamped + 1.0) * gate_clamped * gate_sigmoid).astype(jnp.bfloat16)
    act_grad = lax.dot_general(grad_rows, down_weight, contract, preferred_element_type=jnp.float32)
    gate_grad = jnp.where(gate_pre < CLAMP_LIMIT, act_grad * (up_clamped + 1.0) * gate_sigmoid * (1.0 + SIGMOID_SCALE * gate_clamped * (1.0 - gate_sigmoid)), 0.0).astype(jnp.bfloat16)
    up_grad = jnp.where(jnp.abs(up_pre) < CLAMP_LIMIT, act_grad * gate_clamped * gate_sigmoid, 0.0).astype(jnp.bfloat16)
    grad_down = lax.dot_general(activation, grad_rows, across, preferred_element_type=jnp.float32).astype(jnp.bfloat16)
    grad_gate_w = lax.dot_general(gate_grad, in_rows, across, preferred_element_type=jnp.float32).astype(jnp.bfloat16)
    grad_up_w = lax.dot_general(up_grad, in_rows, across, preferred_element_type=jnp.float32).astype(jnp.bfloat16)
    input_grad = jnp.dot(gate_grad, gate_weight, preferred_element_type=jnp.float32) + jnp.dot(up_grad, up_weight, preferred_element_type=jnp.float32)
    return (grad_gate_w, grad_up_w, grad_down, input_grad)

def reference(mix_values, mix_gate, input_keys, output_keys, step_sizes, decay_rates, out_proj, expert_inputs, stream_grad, routes, route_weights, gate_proj, up_proj, down_proj):
    per_group = HEADS // GROUPS
    head_values = mix_values.astype(jnp.float32).reshape(TOKENS, GROUPS, per_group, HEAD_DIM)
    in_keys = input_keys.astype(jnp.float32).reshape(TOKENS, GROUPS, NSTATE)
    out_keys = output_keys.astype(jnp.float32).reshape(TOKENS, GROUPS, NSTATE)
    head_steps = step_sizes.reshape(TOKENS, GROUPS, per_group)
    head_rates = decay_rates.reshape(GROUPS, per_group)
    start_state = jnp.zeros((GROUPS, per_group, HEAD_DIM, NSTATE), jnp.float32)

    def mixer_only(values_in, keys_in, keys_out, steps_in):
        return decay_span(values_in, keys_in, keys_out, steps_in, head_rates, start_state)[0]
    mixer_out, back_mixer = jax.vjp(mixer_only, head_values, in_keys, out_keys, head_steps)
    gate_in = mix_gate.astype(jnp.float32).reshape(TOKENS, GROUPS, per_group, HEAD_DIM)
    gate_sigmoid = jax.nn.sigmoid(gate_in)
    gate_silu = gate_in * gate_sigmoid
    gated_out = (mixer_out * gate_silu).reshape(TOKENS, DI).astype(jnp.bfloat16)
    flat_routes = routes.reshape(-1)
    one_hot = (flat_routes[:, None] == jnp.arange(EXPERTS, dtype=jnp.int32)[None, :]).astype(jnp.int32)
    slot_rank = lax.optimization_barrier(jnp.sum((jnp.cumsum(one_hot, axis=0) - 1) * one_hot, axis=1))
    expert_slots = N_SP * CAP
    slot_index = (flat_routes * expert_slots + slot_rank).astype(jnp.int32)
    slot_table = jnp.zeros((EXPERTS * expert_slots,), jnp.int32).at[slot_index].set(jnp.arange(TOKENS * TOPK, dtype=jnp.int32) + 1)
    flat_weights = route_weights.reshape(-1)

    def expert_pass(packed):
        slot_routes, gate_weight, up_weight, down_weight = packed
        slot_used = slot_routes > 0
        route_id = jnp.maximum(slot_routes - 1, 0)
        token_id = route_id // TOPK
        route_scale = jnp.where(slot_used, flat_weights[route_id], 0.0)
        grad_rows = (stream_grad[token_id].astype(jnp.float32) * route_scale[:, None]).astype(jnp.bfloat16)
        in_rows = jnp.where(slot_used[:, None], expert_inputs[token_id], jnp.zeros((), jnp.bfloat16))
        return expert_backward(in_rows, grad_rows, gate_weight, up_weight, down_weight)
    grad_gate_proj, grad_up_proj, grad_down_proj, input_grads = lax.map(expert_pass, (slot_table.reshape(EXPERTS, expert_slots), gate_proj, up_proj, down_proj))
    per_route = input_grads.reshape(EXPERTS * expert_slots, D)[slot_index].reshape(TOKENS, TOPK, D)
    stream_total = (stream_grad.astype(jnp.float32) + lax.optimization_barrier(jnp.sum(per_route, axis=1))).astype(jnp.bfloat16)
    across = (((0,), (0,)), ((), ()))
    grad_out_proj = lax.dot_general(stream_total, gated_out, across, preferred_element_type=jnp.float32)
    gated_grad = jnp.dot(stream_total, out_proj, preferred_element_type=jnp.float32).reshape(TOKENS, GROUPS, per_group, HEAD_DIM)
    grad_gate = (gated_grad * mixer_out * gate_sigmoid * (1.0 + gate_in * (1.0 - gate_sigmoid))).reshape(TOKENS, DI).astype(jnp.bfloat16)
    mixer_grad = gated_grad * gate_silu
    grad_vals, grad_in, grad_out, grad_step = back_mixer(mixer_grad)
    return (grad_gate_proj, grad_up_proj, grad_down_proj, grad_out_proj, grad_vals.reshape(TOKENS, DI).astype(jnp.bfloat16), grad_gate, grad_in.reshape(TOKENS, GROUPS * NSTATE).astype(jnp.bfloat16), grad_out.reshape(TOKENS, GROUPS * NSTATE).astype(jnp.bfloat16), grad_step.reshape(TOKENS, HEADS))
```

```python
import functools

import jax
import jax.numpy as jnp
from jax import lax
from jax.experimental import pallas as pl
from jax.experimental.pallas import tpu as pltpu
from jax.sharding import PartitionSpec as P

NSTATE = 128
BLOCK = 128
SP = ("sp",)


CLAMP_LIMIT = 7.0
SIGMOID_SCALE = 1.702


def side_by_side(arrays, axis, split_dim, concat_dim, along):
    both = jnp.concatenate(arrays, axis=along)
    out, at, gathered = (
        lax.all_to_all(both, axis, split_axis=split_dim, concat_axis=concat_dim, tiled=True),
        0,
        [],
    )
    for a in arrays:
        gathered.append(lax.slice_in_dim(out, at, at + a.shape[along], axis=along))
        at += a.shape[along]
    return tuple(gathered)


def in_blocks(x, dim, count):
    lengths = x.shape
    tiles = x.reshape(*lengths[:dim], count, lengths[dim] // count, *lengths[dim + 1 :])
    return jnp.moveaxis(tiles, dim, 0)


def summed_on_arrival(x, axis, dim):
    tiles = in_blocks(x, dim, lax.axis_size(axis))
    arrived = lax.all_to_all(tiles, axis, split_axis=0, concat_axis=0, tiled=True)
    return arrived.astype(jnp.float32).sum(axis=0)


def filled_with(x, identity):
    return jax.tree.map(
        lambda a, e: jnp.broadcast_to(jnp.asarray(e, a.dtype), a.shape), x, identity
    )


def carried_in(x, axes, combine, identity, reverse):
    before = start = filled_with(x, identity)
    so_far = x
    for axis in reversed(axes):
        count, here = (lax.axis_size(axis), lax.axis_index(axis))
        pieces = jax.tree.map(lambda part: lax.all_gather(part, axis), so_far)
        inside, so_far = (start, start)
        for k in reversed(range(count)) if reverse else range(count):
            passed = k > here if reverse else k < here
            so_far = combine(so_far, jax.tree.map(lambda part: part[k], pieces))
            inside = jax.tree.map(lambda new, old: jnp.where(passed, new, old), so_far, inside)
        before = combine(inside, before)
    return before


def decay_span(head_values, in_keys, out_keys, head_steps, head_rates, start_state):
    length = head_values.shape[0]
    num_blocks = length // BLOCK
    causal_mask = jnp.tril(jnp.ones((BLOCK, BLOCK), dtype=bool))

    def advance(carry_state, block_data):
        block_values, block_in, block_out, block_steps = block_data
        log_decay = jnp.cumsum(-block_steps * head_rates, axis=0)
        weighted = block_values * block_steps[..., None]
        ordered = jnp.transpose(log_decay, (1, 2, 0))
        log_gaps = ordered[..., :, None] - ordered[..., None, :]
        mixing = jnp.where(causal_mask, jnp.exp(jnp.where(causal_mask, log_gaps, 0.0)), 0.0)
        scores = jnp.einsum("lgn,sgn->gls", block_out, block_in)
        within = jnp.einsum("grls,sgrp->lgrp", scores[:, None] * mixing, weighted)
        carried = (
            jnp.einsum("lgn,grpn->lgrp", block_out, carry_state) * jnp.exp(log_decay)[..., None]
        )
        to_end = jnp.exp(log_decay[-1] - log_decay)
        new_state = carry_state * jnp.exp(log_decay[-1])[..., None, None] + jnp.einsum(
            "lgn,lgrp->grpn", block_in, weighted * to_end[..., None]
        )
        return (new_state, within + carried)

    blocks = tuple(
        (
            whole_array.reshape((num_blocks, BLOCK) + whole_array.shape[1:])
            for whole_array in (head_values, in_keys, out_keys, head_steps)
        )
    )
    last_state, block_outputs = lax.scan(advance, start_state, blocks)
    return (block_outputs.reshape(head_values.shape), last_state)


MESH_ID = pl.DeviceIdType.MESH
F32 = jnp.float32
BF16 = jnp.bfloat16
COLS = 128
CAP = 12
RING = 4


def nt(a, b):
    return lax.dot_general(a, b, (((1,), (1,)), ((), ())), preferred_element_type=F32)


def tn(a, b):
    return lax.dot_general(a, b, (((0,), (0,)), ((), ())), preferred_element_type=F32)


def nn(a, b):
    return lax.dot_general(a, b, (((1,), (0,)), ((), ())), preferred_element_type=F32)


def iota(shape, dim):
    return lax.broadcasted_iota(jnp.int32, shape, dim)


def up(i, by):
    return lax.rem(i + by, RING)


class Plane:
    def __init__(self, first_is_x):
        tp = lax.axis_index("tp")
        x, y = lax.rem(tp, RING), lax.div(tp, RING)
        self.first_is_x = first_is_x
        self.p, self.q = (x, y) if first_is_x else (y, x)

    def tp_of(self, p, q):
        return q * RING + p if self.first_is_x else p * RING + q

    def at(self, i, j):
        return self.tp_of(up(self.p, i), up(self.q, j))


def remote(src, dst, sems, k, **where):
    send, recv = sems
    return pltpu.make_async_remote_copy(
        src_ref=src,
        dst_ref=dst,
        send_sem=send.at[k],
        recv_sem=recv.at[k],
        device_id=where,
        device_id_type=MESH_ID,
    )


class Gather:
    def __init__(self, plane, buf, row0, rows, sems, base):
        self.plane, self.buf, self.row0, self.rows, self.sems, self.base = plane, buf, row0, rows, sems, base

    def block(self, tp, part):
        start, count = self.row0, self.rows
        if part is not None:
            count = self.rows // 2
            start = start + part * count
        return self.buf.at[pl.ds(start, count), pl.ds(pl.multiple_of(tp * COLS, COLS), COLS)]

    def copy(self, k, i, j, part, di, dj):
        b = self.block(self.plane.at(i, j), part)
        return remote(b, b, self.sems, self.base + k, tp=self.plane.at(di, dj))

    def first(self):
        self.copy(0, 0, 0, None, 1, 0).start()
        self.copy(1, 0, 0, None, 3, 0).start()
        self.second(0)

    def second(self, i):
        n = 4 + 4 * i
        self.copy(n, i, 0, None, 0, 1).start()
        self.copy(n + 1, i, 0, None, 0, 3).start()

    def arrived(self, k, i, j, part):
        self.copy(k, i, j, part, 0, 1).wait_recv()

    def from_low(self):
        self.arrived(0, 3, 0, None)
        self.copy(2, 3, 0, 0, 1, 0).start()
        self.second(3)

    def from_high(self):
        self.arrived(1, 1, 0, None)
        self.copy(3, 1, 0, 1, 3, 0).start()
        self.second(1)

    def opposite(self):
        self.arrived(2, 2, 0, 0)
        self.arrived(3, 2, 0, 1)
        self.second(2)

    def pass_on(self, i):
        n = 4 + 4 * i
        self.arrived(n, i, 3, None)
        self.copy(n + 2, i, 3, 0, 0, 1).start()
        self.arrived(n + 1, i, 1, None)
        self.copy(n + 3, i, 1, 1, 0, 3).start()

    def finish(self):
        for i in (0, 3, 1, 2):
            n = 4 + 4 * i
            self.arrived(n + 2, i, 2, 0)
            self.arrived(n + 3, i, 2, 1)
        self.copy(0, 0, 0, None, 1, 0).wait_send()
        self.copy(1, 0, 0, None, 3, 0).wait_send()
        self.copy(2, 3, 0, 0, 1, 0).wait_send()
        self.copy(3, 1, 0, 1, 3, 0).wait_send()
        for i in (0, 3, 1, 2):
            n = 4 + 4 * i
            self.copy(n, i, 0, None, 0, 1).wait_send()
            self.copy(n + 1, i, 0, None, 0, 3).wait_send()
            self.copy(n + 2, i, 3, 0, 0, 1).wait_send()
            self.copy(n + 3, i, 1, 1, 0, 3).wait_send()


def gather_start(halves):
    for g in halves:
        g.first()


def gather_rest(halves):
    for step in ("from_low", "from_high"):
        for g in halves:
            getattr(g, step)()
    for g in halves:
        g.pass_on(0)
    for g in halves:
        g.opposite()
    for i in (3, 1, 2):
        for g in halves:
            g.pass_on(i)
    for g in halves:
        g.finish()


def split_stage(send, sems, base, bufs, p, to_high, to_low):
    far_low, far_high, low0, low1, high0, high1, sum_up, sum_down = bufs

    def c(k, src, dst, where):
        return remote(src, dst, sems, base + k, tp=where)

    sends = [
        c(0, send(up(p, 2), 0), far_low, to_high),
        c(1, send(up(p, 2), 1), far_high, to_low),
        c(2, send(up(p, 1), 1), low1, to_high),
        c(3, send(up(p, 3), 0), high0, to_low),
        c(4, sum_up, low0, to_high),
        c(5, sum_down, high1, to_low),
    ]

    def start():
        for k in range(4):
            sends[k].start()

    def middle():
        sends[0].wait_recv()
        sum_up[...] = (far_low[...].astype(F32) + send(up(p, 1), 0)[...].astype(F32)).astype(BF16)
        sends[4].start()
        sends[1].wait_recv()
        sum_down[...] = (far_high[...].astype(F32) + send(up(p, 3), 1)[...].astype(F32)).astype(BF16)
        sends[5].start()

    def end():
        for k in (2, 3, 4, 5):
            sends[k].wait_recv()
        lower = send(p, 0)[...].astype(F32) + low0[...].astype(F32) + high0[...].astype(F32)
        upper = send(p, 1)[...].astype(F32) + low1[...].astype(F32) + high1[...].astype(F32)
        return lower, upper

    def drain():
        for k in range(6):
            sends[k].wait_send()

    return start, middle, end, drain


def moe_kernel(
    n_sp,
    routes_ref,
    routes_t_ref,
    route_w_ref,
    rows_ref,
    grad_ref,
    gate_ref,
    up_ref,
    down_ref,
    d_gate_ref,
    d_up_ref,
    d_down_ref,
    total_ref,
    send1,
    recv1,
    all_rows,
    all_grad,
    part0,
    part1,
    far_a0,
    far_a1,
    far_b0,
    far_b1,
    mid0,
    mid1,
    send2,
    recv2,
    s_z1,
    r_z1,
    s_ag,
    r_ag,
    s_rs,
    r_rs,
    s_z2,
    r_z2,
    s_tg,
    r_tg,
):
    sp, tp = lax.axis_index("sp"), lax.axis_index("tp")
    tokens, width = grad_ref.shape
    slots = n_sp * CAP
    planes = (Plane(True), Plane(False))
    barrier = pltpu.get_barrier_semaphore()

    def greet(d, _):
        pl.semaphore_signal(barrier, inc=1, device_id={"sp": lax.rem(sp + d, n_sp)}, device_id_type=MESH_ID)
        return 0

    lax.fori_loop(1, n_sp, greet, 0)
    for i, j in ((1, 0), (3, 0), (0, 1), (0, 3)):
        pl.semaphore_signal(barrier, inc=1, device_id={"tp": planes[0].at(i, j)}, device_id_type=MESH_ID)

    my_cols = pl.ds(pl.multiple_of(tp * COLS, COLS), COLS)
    r_row = routes_t_ref[...]
    expert_rows = iota((n_sp, tokens), 0)
    hit_t = [(expert_rows == r_row[k : k + 1]) for k in range(2)]
    any_t = jnp.where(hit_t[0] | hit_t[1], 1.0, 0.0).astype(BF16)
    before = jnp.where(iota((tokens, tokens), 0) < iota((tokens, tokens), 1), 1.0, 0.0).astype(BF16)
    ranks_t = nn(any_t, before)
    rank_row = [
        jnp.sum(jnp.where(h, ranks_t, 0.0), axis=0, keepdims=True).astype(jnp.int32) for h in hit_t
    ]
    e3 = iota((n_sp, 2 * CAP, tokens), 0)
    c3 = iota((n_sp, 2 * CAP, tokens), 1)
    here = [
        [
            (e3 == r_row[k : k + 1][None]) & (c3 == rank_row[k][None] + shift)
            for k in range(2)
        ]
        for shift in (0, CAP)
    ]

    def pick(mask):
        return jnp.where(mask, 1.0, 0.0).reshape(n_sp * 2 * CAP, tokens).astype(BF16)

    cut = here[0][0] | here[0][1]
    cut = cut & (c3 < CAP)
    my_grad = grad_ref[:, my_cols].astype(F32)
    scaled = [(my_grad * route_w_ref[:, k : k + 1]).astype(BF16) for k in range(2)]
    message = (
        nn(pick(cut), rows_ref[:, my_cols]) + nn(pick(here[1][0]), scaled[0]) + nn(pick(here[1][1]), scaled[1])
    )
    send1[...] = message.astype(BF16).reshape(n_sp, 2 * CAP, COLS)

    pl.semaphore_wait(barrier, n_sp - 1 + 4)

    def z_copy(send, recv, sems, d):
        to = lax.rem(sp + d, n_sp)
        return remote(send.at[to], recv.at[sp], sems, d, sp=to)

    def z_start(send, recv, sems):
        lax.fori_loop(1, n_sp, lambda d, _: (z_copy(send, recv, sems, d).start(), 0)[1], 0)
        recv[pl.ds(sp, 1)] = send[pl.ds(sp, 1)]

    def z_wait(send, recv, sems):
        lax.fori_loop(1, n_sp, lambda d, _: (z_copy(send, recv, sems, d).wait(), 0)[1], 0)

    z_start(send1, recv1, (s_z1, r_z1))

    route_cols = routes_ref[...]
    expert_cols = iota((tokens, n_sp), 1)
    hit = [(expert_cols == route_cols[:, k : k + 1]) for k in range(2)]
    any_c = jnp.where(hit[0] | hit[1], 1.0, 0.0).astype(BF16)
    after = jnp.where(iota((tokens, tokens), 1) < iota((tokens, tokens), 0), 1.0, 0.0).astype(BF16)
    ranks = nn(after, any_c)
    j2 = iota((tokens, n_sp * 16), 1)
    back = None
    for k in range(2):
        rank_col = jnp.sum(jnp.where(hit[k], ranks, 0.0), axis=1, keepdims=True).astype(jnp.int32)
        one = (lax.shift_right_logical(j2, 4) == route_cols[:, k : k + 1]) & ((j2 & 15) == rank_col)
        back = one if back is None else back | one
    back = jnp.where(back, 1.0, 0.0).astype(BF16)

    qi, qj = iota((96, 96), 0), iota((96, 96), 1)
    half = jnp.where(qi >= 48, 1, 0)
    qr = qi - 48 * half
    qs = jnp.where(qr >= 36, 3, jnp.where(qr >= 24, 2, jnp.where(qr >= 12, 1, 0)))
    squeeze = jnp.where(qj == qr + 12 * qs + 12 * half, 1.0, 0.0).astype(BF16)

    z_wait(send1, recv1, (s_z1, r_z1))
    for g in range(n_sp // 4):
        got = recv1[pl.ds(4 * g, 4)].reshape(96, COLS)
        rows = nn(squeeze, got).astype(BF16)
        all_rows[pl.ds(48 * g, 48), my_cols] = rows[:48]
        all_grad[pl.ds(48 * g, 48), my_cols] = rows[48:]

    halves = (
        Gather(planes[0], all_rows, 0, slots, (s_ag, r_ag), 0),
        Gather(planes[1], all_grad, 0, slots, (s_ag, r_ag), 20),
    )
    gather_start(halves)
    gather_rest(halves)

    x = all_rows[...]
    g = all_grad[...]
    gate_pre = nt(x, gate_ref[0])
    up_pre = nt(x, up_ref[0])
    act_grad = nt(g, down_ref[0])
    gate_c = jnp.minimum(gate_pre, CLAMP_LIMIT)
    up_c = jnp.clip(up_pre, -CLAMP_LIMIT, CLAMP_LIMIT)
    sg = jax.nn.sigmoid(SIGMOID_SCALE * gate_c)
    gate_grad = jnp.where(
        gate_pre < CLAMP_LIMIT,
        act_grad * (up_c + 1.0) * sg * (1.0 + SIGMOID_SCALE * gate_c * (1.0 - sg)),
        0.0,
    ).astype(BF16)
    up_grad = jnp.where(jnp.abs(up_pre) < CLAMP_LIMIT, act_grad * gate_c * sg, 0.0).astype(BF16)
    activation = ((up_c + 1.0) * gate_c * sg).astype(BF16)

    mid_row = slots // 2
    for b in range(width // (2 * COLS)):
        cols = pl.ds(2 * COLS * b, 2 * COLS)
        part = (nn(gate_grad, gate_ref[0, :, cols]) + nn(up_grad, up_ref[0, :, cols])).astype(BF16)
        for s in range(2):
            y, xx = divmod(2 * b + s, RING)
            piece = part[:, s * COLS : (s + 1) * COLS]
            part0[xx, y] = piece[:mid_row]
            part1[y, xx] = piece[mid_row:]

    rs = (s_rs, r_rs)
    stages = []
    for h, (plane, part, far) in enumerate(zip(planes, (part0, part1), ((far_a0, far_b0), (far_a1, far_b1)))):
        stages.append(
            split_stage(
                lambda dest, hf, part=part: part.at[dest, pl.ds(2 * hf, 2)],
                rs,
                12 * h,
                [far[0].at[k] for k in range(8)],
                plane.p,
                plane.at(1, 0),
                plane.at(3, 0),
            )
        )
    for st in stages:
        st[0]()
    d_down_ref[0] = tn(activation, g).astype(BF16)
    for st in stages:
        st[1]()
    d_gate_ref[0] = tn(gate_grad, x).astype(BF16)
    second = []
    for h, (plane, mid, far) in enumerate(zip(planes, (mid0, mid1), (far_b0, far_b1))):
        lower, upper = stages[h][2]()
        mid[pl.ds(0, 2)] = lower.astype(BF16)
        mid[pl.ds(2, 2)] = upper.astype(BF16)
        quarter = mid_row // 2
        st = split_stage(
            lambda dest, hf, mid=mid: mid.at[dest, pl.ds(quarter * hf, quarter)],
            rs,
            12 * h + 6,
            [far.at[k] for k in range(8)],
            plane.q,
            plane.at(0, 1),
            plane.at(0, 3),
        )
        st[0]()
        second.append(st)
    d_up_ref[0] = tn(up_grad, x).astype(BF16)
    for st in second:
        st[1]()
    ei, ej = iota((64, 48), 0), iota((64, 48), 1)
    spread = jnp.where(((ei & 15) < CAP) & (ej == lax.shift_right_logical(ei, 4) * CAP + (ei & 15)), 1.0, 0.0)
    spread = spread.astype(BF16)
    for h, st in enumerate(second):
        for hf, piece in enumerate(st[2]()):
            piece = piece.astype(BF16)
            for g2 in range(2):
                at = 4 * (4 * h + 2 * hf + g2)
                send2[pl.ds(at, 4)] = nn(spread, piece[48 * g2 : 48 * (g2 + 1)]).astype(BF16).reshape(4, 16, COLS)

    z_start(send2, recv2, (s_z2, r_z2))
    for st in stages + second:
        st[3]()
    z_wait(send2, recv2, (s_z2, r_z2))
    summed = nn(back, recv2[...].reshape(n_sp * 16, COLS))
    total_ref[:, my_cols] = (my_grad + summed).astype(BF16)
    rows_half = tokens // 2
    tg = (s_tg, r_tg)
    halves = (
        Gather(planes[0], total_ref, 0, rows_half, tg, 0),
        Gather(planes[1], total_ref, rows_half, rows_half, tg, 20),
    )
    gather_start(halves)
    gather_rest(halves)


def expert_part(routes, route_weights, expert_inputs, stream_grad, gate_proj, up_proj, down_proj):
    n_sp = lax.axis_size("sp")
    tokens, width = stream_grad.shape
    slots = n_sp * CAP
    n_tp = RING * RING
    vm = pl.BlockSpec(memory_space=pltpu.VMEM)
    dma = pltpu.SemaphoreType.DMA
    w = jax.ShapeDtypeStruct(gate_proj.shape, BF16)
    return pl.pallas_call(
        functools.partial(moe_kernel, n_sp),
        out_shape=(w, w, w, jax.ShapeDtypeStruct((tokens, width), BF16)),
        in_specs=[vm] * 8,
        out_specs=(vm,) * 4,
        scratch_shapes=[
            pltpu.VMEM((n_sp, 2 * CAP, COLS), BF16),
            pltpu.VMEM((n_sp, 2 * CAP, COLS), BF16),
            pltpu.VMEM((slots, width), BF16),
            pltpu.VMEM((slots, width), BF16),
            pltpu.VMEM((RING, RING, slots // 2, COLS), BF16),
            pltpu.VMEM((RING, RING, slots // 2, COLS), BF16),
            pltpu.VMEM((8, 2, slots // 2, COLS), BF16),
            pltpu.VMEM((8, 2, slots // 2, COLS), BF16),
            pltpu.VMEM((8, slots // 4, COLS), BF16),
            pltpu.VMEM((8, slots // 4, COLS), BF16),
            pltpu.VMEM((RING, slots // 2, COLS), BF16),
            pltpu.VMEM((RING, slots // 2, COLS), BF16),
            pltpu.VMEM((n_sp, 16, COLS), BF16),
            pltpu.VMEM((n_sp, 16, COLS), BF16),
            dma((n_sp,)),
            dma((n_sp,)),
            dma((40,)),
            dma((40,)),
            dma((24,)),
            dma((24,)),
            dma((n_sp,)),
            dma((n_sp,)),
            dma((40,)),
            dma((40,)),
        ],
        compiler_params=pltpu.CompilerParams(
            collective_id=0, has_side_effects=True, vmem_limit_bytes=60 * 1024 * 1024
        ),
        name="experts",
    )(
        routes,
        routes.T,
        route_weights,
        expert_inputs,
        stream_grad,
        gate_proj,
        up_proj,
        down_proj,
    )


def compose(earlier, later):
    return (earlier[0] * later[0], later[0][..., None, None] * earlier[1] + later[1])


def body(
    mix_values,
    mix_gate,
    input_keys,
    output_keys,
    step_sizes,
    decay_rates,
    out_proj,
    expert_inputs,
    stream_grad,
    routes,
    route_weights,
    gate_proj,
    up_proj,
    down_proj,
):
    tok_rows = mix_values.shape[0]
    num_heads = step_sizes.shape[1]
    num_groups = input_keys.shape[1] // NSTATE
    per_group = num_heads // num_groups
    head_size = mix_values.shape[1] // num_heads
    across = (((0,), (0,)), ((), ()))
    grad_gate_proj, grad_up_proj, grad_down_proj, stream_total = expert_part(
        routes, route_weights, expert_inputs, stream_grad, gate_proj, up_proj, down_proj
    )
    head_values = mix_values.astype(jnp.float32).reshape(tok_rows, num_groups, per_group, head_size)
    in_keys = input_keys.astype(jnp.float32).reshape(tok_rows, num_groups, NSTATE)
    out_keys = output_keys.astype(jnp.float32).reshape(tok_rows, num_groups, NSTATE)
    head_steps = step_sizes.reshape(tok_rows, num_groups, per_group)
    head_rates = decay_rates.reshape(num_groups, per_group)
    zero_state = jnp.zeros((num_groups, per_group, head_size, NSTATE), jnp.float32)

    def local_span(values_in, keys_in, keys_out, steps_in):
        return decay_span(values_in, keys_in, keys_out, steps_in, head_rates, zero_state)

    (own_out, own_state), back_local = jax.vjp(
        local_span, head_values, in_keys, out_keys, head_steps
    )
    span_decay = jnp.exp(-jnp.sum(head_steps * head_rates, axis=0))
    identity = (jnp.ones_like(span_decay), jnp.zeros_like(own_state))
    state_in = carried_in((span_decay, own_state), SP, compose, identity, False)[1]

    def entering(state_value, keys_out, steps_in):
        decay_here = jnp.exp(jnp.cumsum(-steps_in * head_rates, axis=0))
        return jnp.einsum("lgn,grpn->lgrp", keys_out, state_value) * decay_here[..., None]

    enter_out, back_enter = jax.vjp(entering, state_in, out_keys, head_steps)
    mixer_out = own_out + enter_out
    gate_in = mix_gate.astype(jnp.float32).reshape(tok_rows, num_groups, per_group, head_size)
    gate_sigmoid = jax.nn.sigmoid(gate_in)
    gate_silu = gate_in * gate_sigmoid
    gated_out = (mixer_out * gate_silu).reshape(tok_rows, -1).astype(jnp.bfloat16)
    stream_part_cols = stream_total
    gated_grad = jnp.dot(
        stream_part_cols,
        lax.all_gather(out_proj, SP, axis=0, tiled=True),
        preferred_element_type=jnp.float32,
    )
    gated_grad = gated_grad.reshape(tok_rows, num_groups, per_group, head_size)
    grad_gate = (
        (gated_grad * mixer_out * gate_sigmoid * (1.0 + gate_in * (1.0 - gate_sigmoid)))
        .reshape(tok_rows, -1)
        .astype(jnp.bfloat16)
    )
    mixer_grad = gated_grad * gate_silu
    state_grad, keys_grad_enter, steps_grad_enter = back_enter(mixer_grad)
    state_out_grad = carried_in((span_decay, state_grad), SP, compose, identity, True)[1]
    grad_vals, grad_in, keys_grad_own, steps_grad_own = back_local((mixer_grad, state_out_grad))
    decay_grad = -head_rates * span_decay * jnp.sum(state_out_grad * state_in, axis=(2, 3))
    grad_steps = (steps_grad_own + steps_grad_enter + decay_grad[None]).reshape(tok_rows, num_heads)
    stream_part_cols = stream_total
    grad_out_proj = summed_on_arrival(
        lax.dot_general(
            stream_part_cols, gated_out, across, preferred_element_type=jnp.float32
        ).astype(jnp.bfloat16),
        SP,
        0,
    )
    return (
        grad_gate_proj,
        grad_up_proj,
        grad_down_proj,
        grad_out_proj,
        grad_vals.reshape(tok_rows, -1).astype(jnp.bfloat16),
        grad_gate,
        grad_in.reshape(tok_rows, -1).astype(jnp.bfloat16),
        (keys_grad_own + keys_grad_enter).reshape(tok_rows, -1).astype(jnp.bfloat16),
        grad_steps,
    )


def solution(mesh):
    in_specs = (
        P(SP, "tp"),
        P(SP, "tp"),
        P(SP, "tp"),
        P(SP, "tp"),
        P(SP, "tp"),
        P("tp"),
        P(SP, "tp"),
        P(SP, None),
        P(SP, None),
        P(SP, None),
        P(SP, None),
        P(SP, "tp", None),
        P(SP, "tp", None),
        P(SP, "tp", None),
    )
    out_specs = (
        P(SP, "tp", None),
        P(SP, "tp", None),
        P(SP, "tp", None),
        P(SP, "tp"),
        P(SP, "tp"),
        P(SP, "tp"),
        P(SP, "tp"),
        P(SP, "tp"),
        P(SP, "tp"),
    )
    return jax.shard_map(body, mesh=mesh, in_specs=in_specs, out_specs=out_specs, check_vma=False)
```
